32 devices in a mesh: ep: 8 (over z, x), tp: 4 (over y, core).
Axes of the slice: x: 2, y: 2, z: 4, core: 2. Of those that a mesh axis runs over, the one named last changes fastest.
Arguments:
- tokens: bfloat16 [2048, 4096], P('ep', 'tp'), may hold values from -72 to 72
- pre_gain: float32 [4096], P('tp'), may hold values from 0.1 to 1.9
- expert_ids: int32 [2048, 3], P('ep'), may hold values from 0 to 15, all different within a row; in each aligned block of 256 rows (0 to 255, 256 to 511, ...) at most 64 rows name the same one
- route_weight: float32 [2048, 3], P('ep'), may hold values from 0.2 to 2
- expert_gate: bfloat16 [16, 1024, 4096], P('ep', 'tp'), may hold values from -0.09375 to 0.09375
- expert_up: bfloat16 [16, 1024, 4096], P('ep', 'tp'), may hold values from -0.09375 to 0.09375
- expert_down: bfloat16 [16, 1024, 4096], P('ep', None, 'tp'), may hold values from -0.9375 to 0.9375
- shared_gate: bfloat16 [1024, 4096], P('tp'), may hold values from -0.09375 to 0.09375
- shared_up: bfloat16 [1024, 4096], P('tp'), may hold values from -0.09375 to 0.09375
- shared_down: bfloat16 [1024, 4096], P(None, 'tp'), may hold values from -0.9375 to 0.9375
- out_gain: float32 [4096], P('tp'), may hold values from 0.1 to 1.9
Outputs:
- mixed: bfloat16 [2048, 4096], P('ep', 'tp')
The draws below stay inside these ranges and needn't reach their ends.
Inputs may be any that keep to these rules, and one draw needn't show every extreme that they name: `expert_ids`: A row names 3 different experts. Among the rows of one index of ep no expert is named more than 64 times, and in every draw some expert is named exactly 64 times there.
All inputs are finite; a program needn't handle non-finite values.
Results may differ from the reference program's by a relative error of at most 0.0068.
Values may be sent and summed in bfloat16 or wider, within the bound.
A program may use at most 64 MiB of HBM per device.

```python
import math
import jax
import jax.numpy as jnp
import numpy as np
from jax import lax

D = 4096
F = 1024
FS = 1024
TOK = 256
TOP = 3
EXPERTS = 16
CAP = 64
TOKENS = 2048
N_EP = 8


def column_ramp(key, top_ratio):
    ramp = jnp.exp(jnp.linspace(0.0, math.log(top_ratio), D)).astype(jnp.float32)
    rough = jax.random.uniform(key, (D,), jnp.float32, 0.5, 1.5)
    return ramp * rough


def base_values(key, shape):
    values = jnp.clip(jax.random.normal(key, shape, jnp.float32), -4.0, 4.0)
    return values


def draw_tokens(key, part):
    key_col, key_row, key_val = jax.random.split(jax.random.fold_in(key, 101), 3)
    column = column_ramp(key_col, 6.0)
    row_scale = jnp.exp(jax.random.uniform(key_row, (TOKENS, 1), jnp.float32, 0.0, math.log(8.0)))
    values = base_values(key_val, (TOKENS, D))
    return (values * column[None, :] * row_scale * 0.25).astype(jnp.bfloat16)


def draw_expert_down(key, part):
    key_col, key_val = jax.random.split(jax.random.fold_in(key, 202), 2)
    column = column_ramp(key_col, 5.0)
    values = base_values(key_val, (EXPERTS, F, D))
    return (values * column[None, None, :] * F ** (-0.5)).astype(jnp.bfloat16)


def draw_shared_down(key, part):
    key_col, key_val = jax.random.split(jax.random.fold_in(key, 303), 2)
    column = column_ramp(key_col, 5.0)
    values = base_values(key_val, (FS, D))
    return (values * column[None, :] * FS ** (-0.5)).astype(jnp.bfloat16)


def block_scale(stream_key, dims, shards, least, top_value):
    level, own = 1.0, jax.random.fold_in(stream_key, 6)
    for axis_at, parts in shards:
        draws = jnp.exp(jax.random.uniform(jax.random.fold_in(own, axis_at), (parts,), jnp.float32, least / len(shards), top_value / len(shards)))
        level = level * jnp.repeat(draws, dims[axis_at] // parts).reshape([-1 if axis == axis_at else 1 for axis in range(len(dims))])
    return level


def deal_out(own_key, own, number, rows, amount, top, reach, skew):
    ranking = jax.random.permutation(own_key, amount)
    heavy_load, common = portions_of(amount, rows * top, reach, skew, True), portions_of(amount, rows * top, reach, skew, False)
    places = jnp.arange(amount)

    def named(sizes, offset_by):
        used = int((sizes > 0).sum())
        fixed = max(1, used // 4)
        moved = fixed + (places - fixed + offset_by * (used - fixed)) % max(1, amount - fixed)
        return jnp.zeros((amount,), jnp.int32).at[ranking[jnp.where(places < fixed, places, moved)]].set(jnp.asarray(sizes, jnp.int32))

    sizes = jnp.where(number % 4 == 0, named(heavy_load, number // 4), named(common, number - number // 4 - 1))
    mixed = jax.random.permutation(jax.random.fold_in(own, 3), amount)
    donor, sink = mixed[0:amount // 2 * 2:2], mixed[1:amount // 2 * 2:2]
    room = jnp.minimum(sizes[donor] - 1, reach - sizes[sink]) // 2
    room = jnp.where((donor == ranking[0]) | (sink == ranking[0]) | (sizes[sink] == 0), 0, jnp.maximum(room, 0))
    moved = jax.random.randint(jax.random.fold_in(own, 4), (amount // 2,), 0, 1 << 20) % (room + 1)
    sizes = sizes.at[donor].add(-moved).at[sink].add(moved)
    members = jnp.searchsorted(jnp.cumsum(sizes), jnp.arange(rows * top), side="right").astype(jnp.int32)
    table = members.reshape(top, rows).T
    table = table[jax.random.permutation(jax.random.fold_in(own, 1), rows)]
    offset_by = jax.random.randint(jax.random.fold_in(own, 2), (rows, 1), 0, top)
    return jnp.take_along_axis(table, (jnp.arange(top)[None, :] + offset_by) % top, axis=1)


def portions_of(count, total, bound, skew, full):
    portions = [(1 << 20) // math.isqrt(standing ** skew) + 1 for standing in range(1, count + 1)]
    largest = bound if full else min(bound, max(-(-total // count), total * portions[0] // sum(portions)))
    least = 1 if total - largest >= count - 1 else 0
    counts, spare = [largest] + [least] * (count - 1), total - largest - least * (count - 1)
    while spare > 0:
        candidates = [i for i in range(1, count) if counts[i] < largest] or [i for i in range(1, count) if counts[i] < bound]
        whole, remaining = sum([portions[i] for i in candidates]), spare
        for i in candidates:
            more = min(bound - counts[i], max(1, remaining * portions[i] // whole), spare)
            counts[i] = counts[i] + more
            spare = spare - more
    return np.array(counts)


def normal_values(key, extent, spread, bound, cuts=(), held_as=jnp.bfloat16):
    level = block_scale(key, extent, cuts, -0.22, 0.18) if cuts else 1.0
    result = jax.random.normal(key, extent, jnp.float32) * spread * level
    return jnp.minimum(jnp.maximum(result, -bound), bound).astype(held_as)


def setup_inputs(seed: int = 0) -> dict:
    key_of = jax.random.split(jax.random.key(seed), 12)
    tokens = draw_tokens(jax.random.fold_in(key_of[11], 71), 0)
    pre_gain = jnp.clip(1.0 + 0.18 * jax.random.normal(key_of[1], (D,), jnp.float32), 0.1, 1.9)
    expert_ids_keys = jax.random.split(jax.random.fold_in(key_of[2], 1), TOKENS // TOK)
    expert_ids_turns = jax.random.permutation(jax.random.fold_in(key_of[2], 3), TOKENS // TOK)
    expert_ids = jax.vmap(lambda own, number: deal_out(jax.random.fold_in(key_of[2], 2), own, number, TOK, EXPERTS, TOP, CAP, 2))(expert_ids_keys, expert_ids_turns).reshape((TOKENS, TOP))
    route_weight = jnp.clip(jnp.exp(math.log(2.0) - 2.3025851 * jax.random.uniform(key_of[3], (TOKENS, TOP), jnp.float32) ** block_scale(key_of[3], (TOKENS, TOP), ((0, 8),), -0.2, 0.2)), 0.2, 2.0)
    expert_gate = normal_values(key_of[4], (EXPERTS, F, D), D ** -0.5, 0.09375, ((0, 8), (1, 4)))
    expert_up = normal_values(key_of[5], (EXPERTS, F, D), D ** -0.5, 0.09375, ((0, 8), (1, 4)))
    expert_down = draw_expert_down(jax.random.fold_in(key_of[11], 71), 0)
    shared_gate = normal_values(key_of[7], (FS, D), D ** -0.5, 0.09375, ((0, 4),))
    shared_up = normal_values(key_of[8], (FS, D), D ** -0.5, 0.09375, ((0, 4),))
    shared_down = draw_shared_down(jax.random.fold_in(key_of[11], 71), 0)
    out_gain = jnp.clip(1.0 + 0.18 * jax.random.normal(key_of[10], (D,), jnp.float32), 0.1, 1.9)
    return {"tokens": tokens, "pre_gain": pre_gain, "expert_ids": expert_ids, "route_weight": route_weight, "expert_gate": expert_gate, "expert_up": expert_up, "expert_down": expert_down, "shared_gate": shared_gate, "shared_up": shared_up, "shared_down": shared_down, "out_gain": out_gain}


EPSILON = 1e-06

def norm_rows(values, gain):
    scale = lax.rsqrt(lax.optimization_barrier(jnp.mean(values * values, axis=-1, keepdims=True)) + EPSILON)
    return values * scale * gain

def reference(tokens, pre_gain, expert_ids, route_weight, expert_gate, expert_up, expert_down, shared_gate, shared_up, shared_down, out_gain):
    normed = norm_rows(tokens.astype(jnp.float32), pre_gain).astype(jnp.bfloat16)
    flat_ids = expert_ids.reshape(N_EP, TOK * TOP).astype(jnp.int32)
    one_hot = (flat_ids[:, :, None] == jnp.arange(EXPERTS, dtype=jnp.int32)[None, None, :]).astype(jnp.int32)
    before = jnp.cumsum(one_hot, axis=1) - one_hot
    slot_index = lax.optimization_barrier(jnp.sum(before * one_hot, axis=2)).astype(jnp.int32)
    dest_index = (flat_ids * CAP + slot_index).astype(jnp.int32)
    block_index = jnp.arange(N_EP, dtype=jnp.int32)[:, None]
    order = jnp.broadcast_to(jnp.arange(TOK * TOP, dtype=jnp.int32)[None, :], (N_EP, TOK * TOP))
    source = jnp.full((N_EP, EXPERTS * CAP), -1, jnp.int32).at[block_index, dest_index].set(order)
    is_live = source >= 0
    row_index = (jnp.where(is_live, source // TOP, 0) + block_index * TOK).astype(jnp.int32)
    row_index = row_index.reshape(N_EP, EXPERTS, CAP).transpose(1, 0, 2).reshape(EXPERTS, N_EP * CAP)
    is_live = is_live.reshape(N_EP, EXPERTS, CAP).transpose(1, 0, 2).reshape(EXPERTS, N_EP * CAP)

    def one_expert(operands):
        expert_rows, expert_live, weight_gate, weight_up, weight_down = operands
        buffer = normed[expert_rows] * expert_live[:, None].astype(jnp.bfloat16)
        gate_sum = jnp.dot(buffer, weight_gate.T, preferred_element_type=jnp.float32)
        up_sum = jnp.dot(buffer, weight_up.T, preferred_element_type=jnp.float32)
        hidden_act = (jax.nn.silu(gate_sum) * up_sum).astype(jnp.bfloat16)
        return jnp.dot(hidden_act, weight_down, preferred_element_type=jnp.float32).astype(jnp.bfloat16)
    results = lax.map(one_expert, (row_index, is_live, expert_gate, expert_up, expert_down))
    results = results.reshape(EXPERTS * N_EP * CAP, D)
    lookup = (flat_ids * (N_EP * CAP) + block_index * CAP + slot_index).reshape(TOKENS * TOP).astype(jnp.int32)
    picked = results[lookup].reshape(TOKENS, TOP, D).astype(jnp.float32)
    routed = lax.optimization_barrier(jnp.sum(picked * route_weight[:, :, None], axis=1))
    shared_gate_sum = jnp.dot(normed, shared_gate.T, preferred_element_type=jnp.float32)
    shared_up_sum = jnp.dot(normed, shared_up.T, preferred_element_type=jnp.float32)
    shared_act = (jax.nn.silu(shared_gate_sum) * shared_up_sum).astype(jnp.bfloat16)
    shared_out = jnp.dot(shared_act, shared_down, preferred_element_type=jnp.float32)
    summed = routed + shared_out
    return norm_rows(summed, out_gain).astype(jnp.bfloat16)
```

```python
import functools

import jax
import jax.numpy as jnp
from jax import lax
from jax.experimental import pallas as pl
from jax.experimental.pallas import tpu as pltpu
from jax.sharding import PartitionSpec as P

EPSILON = 1e-06
MESH = pl.DeviceIdType.MESH
GROUPS = 4
CHUNKS = 8


def step_order(n_ep):
    half = n_ep // 2
    far = [half + (half // 2 + k) % half for k in range(half)]
    near = list(range(2, half))
    order = [0, 1]
    while far or near:
        if far:
            order.append(far.pop(0))
        if near:
            order.append(near.pop(0))
    return order


def xor(i, d):
    out = i
    bit = 1
    while bit <= d:
        if d & bit:
            out = out + bit * (1 - 2 * ((i // bit) % 2))
        bit *= 2
    return out


def dot_t(a, b):
    return lax.dot_general(a, b, (((1,), (1,)), ((), ())), preferred_element_type=jnp.float32)


def dot(a, b):
    return jnp.dot(a, b, preferred_element_type=jnp.float32)


def act(gate, up):
    return (gate / (1.0 + jnp.exp(-gate)) * up).astype(jnp.bfloat16)


class Gather:
    def __init__(self, place, source, at, sems, number):
        i, y, c, n_y = place
        ys, yr, ps, pr = sems
        own = y * 2 + c
        partner = (i, y * 2 + (1 - c))
        self.far, self.near = [], []

        def copy(src, dst, s, r, dev):
            return pltpu.make_async_remote_copy(
                src_ref=src, dst_ref=dst, send_sem=s, recv_sem=r, device_id=dev, device_id_type=MESH
            )

        for k in range(1, n_y):
            dev = (i, lax.rem(y + k, n_y) * 2 + c)
            n = number * (n_y - 1) + k - 1
            self.far.append(copy(source, at(own), ys.at[n], yr.at[n], dev))
        self.near.append(copy(source, at(own), ps.at[number * n_y], pr.at[number * n_y], partner))
        for k in range(1, n_y):
            held = at(lax.rem(y + n_y - k, n_y) * 2 + c)
            n = number * n_y + k
            self.near.append(copy(held, held, ps.at[n], pr.at[n], partner))

    def start(self):
        for copy in self.far:
            copy.start()
        self.near[0].start()

    def relay(self):
        for k, copy in enumerate(self.far):
            copy.wait_recv()
            self.near[k + 1].start()

    def finish(self):
        for copy in self.near:
            copy.wait_recv()

    def drain(self):
        for copy in self.far + self.near:
            copy.wait_send()


def kernel(
    n_ep, n_tp, out_ref, norm_ref, whi_ref, wlo_ref, g_hbm, u_hbm, d_hbm, sg_hbm, su_hbm, sd_hbm,
    res_ref,
    seg, sseg, hid, shid, oexp, ret, gw, uw, dw, sgw, suw, sdw,
    wsem, lsem, ds, dr, rs, rr, fys, fyr, fps, fpr, hys, hyr, hps, hpr, sys_, syr, sps, spr,
):
    i, t = lax.axis_index("ep"), lax.axis_index("tp")
    n_y = n_tp // 2
    y, c = t // 2, lax.rem(t, 2)
    place = (i, y, c, n_y)
    own = y * 2 + c
    order = step_order(n_ep)
    _, exp_dev, cap, feat = out_ref.shape
    hidden = gw.shape[1]
    s_hidden = sgw.shape[0]

    loads = [
        pltpu.make_async_copy(a, b, wsem.at[k])
        for k, (a, b) in enumerate(
            ((sg_hbm, sgw), (su_hbm, suw), (g_hbm, gw), (u_hbm, uw), (d_hbm, dw), (sd_hbm, sdw))
        )
    ]
    for load in loads:
        load.start()

    barrier = pltpu.get_barrier_semaphore()
    peers = [(xor(i, d), t) for d in order[1:]]
    peers += [(i, lax.rem(y + k, n_y) * 2 + c) for k in range(1, n_y)]
    peers += [(i, y * 2 + (1 - c))]
    for dev in peers:
        pl.semaphore_signal(barrier, inc=1, device_id=dev, device_id_type=MESH)
    pl.semaphore_wait(barrier, len(peers))

    sends = [None]
    for q in range(1, n_ep):
        sends.append(
            pltpu.make_async_remote_copy(
                src_ref=out_ref.at[q], dst_ref=seg.at[own, :, pl.ds(q * cap, cap), :],
                send_sem=ds.at[q], recv_sem=dr.at[q], device_id=(xor(i, order[q]), t),
                device_id_type=MESH,
            )
        )
    shared = Gather(place, norm_ref, lambda k: sseg.at[k], (sys_, syr, sps, spr), 0)
    for q in range(1, n_ep):
        sends[q].start()
    shared.start()
    stay = pltpu.make_async_copy(out_ref.at[0], seg.at[own, :, pl.ds(0, cap), :], lsem.at[0])
    stay_shared = pltpu.make_async_copy(norm_ref, sseg.at[own], lsem.at[1])
    stay.start()
    stay_shared.start()
    stay.wait()

    per_chunk = n_ep // CHUNKS
    chunk_rows = per_chunk * cap
    rows = n_ep * cap // GROUPS
    chunks = []
    for k in range(CHUNKS):
        at = functools.partial(
            lambda k, j: seg.at[j, :, pl.ds(k * chunk_rows, chunk_rows), :], k
        )
        chunks.append(Gather(place, at(own), at, (fys, fyr, fps, fpr), k))
    acts = []
    for g in range(GROUPS):
        at = functools.partial(lambda g, j: hid.at[j, :, pl.ds(g * rows, rows), :], g)
        acts.append(Gather(place, at(own), at, (hys, hyr, hps, hpr), g))
    shared_act = Gather(place, shid.at[own], lambda k: shid.at[k], (sys_, syr, sps, spr), 1)

    def begin(k):
        for q in range(k * per_chunk, (k + 1) * per_chunk):
            if q:
                sends[q].wait_recv()
        chunks[k].start()

    def gate_up(g):
        for k in range(g * CHUNKS // GROUPS, (g + 1) * CHUNKS // GROUPS):
            chunks[k].finish()
        part = pl.ds(g * rows, rows)

        @pl.loop(0, exp_dev)
        def _(e):
            gate = up = None
            for k in range(n_tp):
                x = seg[k, e, part, :]
                a = dot_t(x, gw[e, :, k * feat:(k + 1) * feat])
                b = dot_t(x, uw[e, :, k * feat:(k + 1) * feat])
                gate = a if gate is None else gate + a
                up = b if up is None else up + b
            hid[own, e, part, :] = act(gate, up)

        acts[g].start()

    per_group = n_ep // GROUPS
    returns = []

    def down(g):
        acts[g].relay()
        acts[g].finish()
        part = pl.ds(g * rows, rows)

        @pl.loop(0, exp_dev)
        def _(e):
            total = None
            for k in range(n_tp):
                a = dot(hid[k, e, part, :], dw[e, k * hidden:(k + 1) * hidden, :])
                total = a if total is None else total + a
            oexp[e, part, :] = total.astype(jnp.bfloat16)

        for q in range(g * per_group, (g + 1) * per_group):
            src = oexp.at[:, pl.ds(q * cap, cap), :]
            if q == 0:
                copy = pltpu.make_async_copy(src, ret.at[0], lsem.at[0])
            else:
                copy = pltpu.make_async_remote_copy(
                    src_ref=src, dst_ref=ret.at[q], send_sem=rs.at[q], recv_sem=rr.at[q],
                    device_id=(xor(i, order[q]), t), device_id_type=MESH,
                )
            copy.start()
            returns.append(copy)

    begin(0)
    begin(1)
    shared.relay()
    chunks[0].relay()
    stay_shared.wait()
    shared.finish()
    loads[0].wait()
    loads[1].wait()
    gate = up = None
    for k in range(n_tp):
        x = sseg[k]
        a = dot_t(x, sgw[:, k * feat:(k + 1) * feat])
        b = dot_t(x, suw[:, k * feat:(k + 1) * feat])
        gate = a if gate is None else gate + a
        up = b if up is None else up + b
    shid[own] = act(gate, up)
    shared_act.start()
    loads[2].wait()
    loads[3].wait()
    loads[4].wait()
    loads[5].wait()
    span = CHUNKS // GROUPS
    for k in range(2, CHUNKS):
        begin(k)
        chunks[k - 1].relay()
        if k % span == span - 1:
            g = k // span - 1
            gate_up(g)
            if g:
                down(g - 1)
    chunks[CHUNKS - 1].relay()
    gate_up(GROUPS - 1)
    down(GROUPS - 2)
    shared_act.relay()
    down(GROUPS - 1)
    shared_act.finish()
    total = None
    for k in range(n_tp):
        a = dot(shid[k], sdw[k * s_hidden:(k + 1) * s_hidden, :])
        total = a if total is None else total + a
    res_ref[...] = total
    width = per_group * exp_dev * cap
    for g in range(GROUPS):
        for q in range(g * per_group, (g + 1) * per_group):
            if q:
                returns[q].wait_recv()
            else:
                returns[q].wait()
        piece = ret[g * per_group:(g + 1) * per_group].reshape(width, feat)
        cols = pl.ds(g * width, width)
        res_ref[...] += dot(whi_ref[:, cols], piece) + dot(wlo_ref[:, cols], piece)
    for q in range(1, n_ep):
        sends[q].wait_send()
        returns[q].wait_send()
    for gather in chunks + acts + [shared, shared_act]:
        gather.drain()


def exchange(n_ep, n_tp, outgoing, normed, whi, wlo, gate, up, down, s_gate, s_up, s_down):
    exp_dev, hidden, width = gate.shape
    _, _, cap, feat = outgoing.shape
    tok = normed.shape[0]
    s_hidden = s_gate.shape[0]
    n_y = n_tp // 2
    bf = jnp.bfloat16
    dma = pltpu.SemaphoreType.DMA
    far, near = n_y - 1, n_y
    vmem, hbm = pl.BlockSpec(memory_space=pltpu.VMEM), pl.BlockSpec(memory_space=pl.ANY)
    return pl.pallas_call(
        functools.partial(kernel, n_ep, n_tp),
        out_shape=jax.ShapeDtypeStruct((tok, feat), jnp.float32),
        in_specs=[vmem] * 4 + [hbm] * 6,
        out_specs=vmem,
        scratch_shapes=[
            pltpu.VMEM((n_tp, exp_dev, n_ep * cap, feat), bf),
            pltpu.VMEM((n_tp, tok, feat), bf),
            pltpu.VMEM((n_tp, exp_dev, n_ep * cap, hidden), bf),
            pltpu.VMEM((n_tp, tok, s_hidden), bf),
            pltpu.VMEM((exp_dev, n_ep * cap, feat), bf),
            pltpu.VMEM((n_ep, exp_dev, cap, feat), bf),
            pltpu.VMEM(gate.shape, bf),
            pltpu.VMEM(up.shape, bf),
            pltpu.VMEM(down.shape, bf),
            pltpu.VMEM(s_gate.shape, bf),
            pltpu.VMEM(s_up.shape, bf),
            pltpu.VMEM(s_down.shape, bf),
            dma((6,)), dma((2,)),
            dma((n_ep,)), dma((n_ep,)), dma((n_ep,)), dma((n_ep,)),
            dma((CHUNKS * far,)), dma((CHUNKS * far,)), dma((CHUNKS * near,)), dma((CHUNKS * near,)),
            dma((GROUPS * far,)), dma((GROUPS * far,)), dma((GROUPS * near,)), dma((GROUPS * near,)),
            dma((2 * far,)), dma((2 * far,)), dma((2 * near,)), dma((2 * near,)),
        ],
        compiler_params=pltpu.CompilerParams(
            collective_id=0, has_side_effects=True, vmem_limit_bytes=56 * 1024 * 1024
        ),
    )(outgoing, normed, whi, wlo, gate, up, down, s_gate, s_up, s_down)


def on_device(
    n_ep, n_tp, tokens, pre_gain, expert_ids, route_weight, expert_gate, expert_up, expert_down,
    shared_gate, shared_up, shared_down, out_gain,
):
    tok_count, top_count = expert_ids.shape
    exp_dev = expert_gate.shape[0]
    width = expert_gate.shape[2]
    experts = exp_dev * n_ep
    capacity = 4 * tok_count * top_count // (3 * experts)
    feat = tokens.shape[1]
    tok_float = tokens.astype(jnp.float32)
    square_sum = lax.psum(jnp.sum(tok_float * tok_float, axis=1), "tp")
    normed = (tok_float * lax.rsqrt(square_sum[:, None] / width + EPSILON) * pre_gain).astype(
        jnp.bfloat16
    )
    i = lax.axis_index("ep")
    steps = jnp.array(step_order(n_ep), jnp.int32)
    names = ((i ^ steps)[:, None] * exp_dev + jnp.arange(exp_dev, dtype=jnp.int32)).reshape(experts)
    same = expert_ids[:, :, None] == names[None, None, :]
    member = jnp.any(same, axis=1)
    weight = jnp.sum(jnp.where(same, route_weight[:, :, None], 0.0), axis=1)
    row = jnp.arange(tok_count, dtype=jnp.int32)
    earlier = (row[None, :] < row[:, None]).astype(jnp.bfloat16)
    before = jnp.dot(earlier, member.astype(jnp.bfloat16), preferred_element_type=jnp.float32)
    slot = jnp.where(member, before.astype(jnp.int32), -1)
    places = jnp.arange(capacity, dtype=jnp.int32)
    pick = (slot.T[:, None, :] == places[None, :, None]).astype(jnp.bfloat16)
    outgoing = jnp.dot(
        pick.reshape(experts * capacity, tok_count), normed, preferred_element_type=jnp.float32
    ).astype(jnp.bfloat16)
    outgoing = outgoing.reshape(n_ep, exp_dev, capacity, feat)
    high = lax.reduce_precision(weight, 8, 7)
    low = weight - high
    here = slot[:, :, None] == places[None, None, :]

    def spread(values):
        return jnp.where(here, values[:, :, None], 0.0).astype(jnp.bfloat16).reshape(
            tok_count, experts * capacity
        )

    summed = exchange(
        n_ep, n_tp, outgoing, normed, spread(high), spread(low), expert_gate, expert_up,
        expert_down, shared_gate, shared_up, shared_down,
    )
    out_square = lax.psum(jnp.sum(summed * summed, axis=1), "tp")
    return (summed * lax.rsqrt(out_square[:, None] / width + EPSILON) * out_gain).astype(
        jnp.bfloat16
    )


def solution(mesh):
    return jax.shard_map(
        functools.partial(on_device, mesh.shape["ep"], mesh.shape["tp"]),
        mesh=mesh,
        in_specs=(
            P("ep", "tp"),
            P("tp"),
            P("ep", None),
            P("ep", None),
            P("ep", "tp", None),
            P("ep", "tp", None),
            P("ep", None, "tp"),
            P("tp", None),
            P("tp", None),
            P(None, "tp"),
            P("tp"),
        ),
        out_specs=P("ep", "tp"),
        check_vma=False,
    )
```

```python
import functools

import jax
import jax.numpy as jnp
from jax import lax
from jax.experimental import pallas as pl
from jax.experimental.pallas import tpu as pltpu
from jax.sharding import PartitionSpec as P

EPSILON = 1e-06
MESH = pl.DeviceIdType.MESH
GROUPS = 4
CHUNKS = 8


def step_order(n_ep):
    half = n_ep // 2
    far = [half + (half // 2 + k) % half for k in range(half)]
    return [0, 1] + far + list(range(2, half))


def xor(i, d):
    out = i
    bit = 1
    while bit <= d:
        if d & bit:
            out = out + bit * (1 - 2 * ((i // bit) % 2))
        bit *= 2
    return out


def dot_t(a, b):
    return lax.dot_general(a, b, (((1,), (1,)), ((), ())), preferred_element_type=jnp.float32)


def dot(a, b):
    return jnp.dot(a, b, preferred_element_type=jnp.float32)


def act(gate, up):
    return (gate / (1.0 + jnp.exp(-gate)) * up).astype(jnp.bfloat16)


class Gather:
    def __init__(self, place, source, at, sems, number):
        i, y, c, n_y = place
        ys, yr, ps, pr = sems
        own = y * 2 + c
        partner = (i, y * 2 + (1 - c))
        self.far, self.near = [], []

        def copy(src, dst, s, r, dev):
            return pltpu.make_async_remote_copy(
                src_ref=src, dst_ref=dst, send_sem=s, recv_sem=r, device_id=dev, device_id_type=MESH
            )

        for k in range(1, n_y):
            dev = (i, lax.rem(y + k, n_y) * 2 + c)
            n = number * (n_y - 1) + k - 1
            self.far.append(copy(source, at(own), ys.at[n], yr.at[n], dev))
        self.near.append(copy(source, at(own), ps.at[number * n_y], pr.at[number * n_y], partner))
        for k in range(1, n_y):
            held = at(lax.rem(y + n_y - k, n_y) * 2 + c)
            n = number * n_y + k
            self.near.append(copy(held, held, ps.at[n], pr.at[n], partner))

    def start(self):
        for copy in self.far:
            copy.start()
        self.near[0].start()

    def relay(self):
        for k, copy in enumerate(self.far):
            copy.wait_recv()
            self.near[k + 1].start()

    def finish(self):
        for copy in self.near:
            copy.wait_recv()

    def drain(self):
        for copy in self.far + self.near:
            copy.wait_send()


def kernel(
    n_ep, n_tp, out_ref, norm_ref, whi_ref, wlo_ref, g_hbm, u_hbm, d_hbm, sg_hbm, su_hbm, sd_hbm,
    res_ref,
    seg, sseg, hid, shid, oexp, ret, gw, uw, dw, sgw, suw, sdw,
    wsem, lsem, ds, dr, rs, rr, fys, fyr, fps, fpr, hys, hyr, hps, hpr, sys_, syr, sps, spr,
):
    i, t = lax.axis_index("ep"), lax.axis_index("tp")
    n_y = n_tp // 2
    y, c = t // 2, lax.rem(t, 2)
    place = (i, y, c, n_y)
    own = y * 2 + c
    order = step_order(n_ep)
    _, exp_dev, cap, feat = out_ref.shape
    hidden = gw.shape[1]
    s_hidden = sgw.shape[0]

    loads = [
        pltpu.make_async_copy(a, b, wsem.at[k])
        for k, (a, b) in enumerate(
            ((sg_hbm, sgw), (su_hbm, suw), (g_hbm, gw), (u_hbm, uw), (d_hbm, dw), (sd_hbm, sdw))
        )
    ]
    for load in loads:
        load.start()

    barrier = pltpu.get_barrier_semaphore()
    peers = [(xor(i, d), t) for d in order[1:]]
    peers += [(i, lax.rem(y + k, n_y) * 2 + c) for k in range(1, n_y)]
    peers += [(i, y * 2 + (1 - c))]
    for dev in peers:
        pl.semaphore_signal(barrier, inc=1, device_id=dev, device_id_type=MESH)
    pl.semaphore_wait(barrier, len(peers))

    sends = [None]
    for q in range(1, n_ep):
        sends.append(
            pltpu.make_async_remote_copy(
                src_ref=out_ref.at[q], dst_ref=seg.at[own, :, pl.ds(q * cap, cap), :],
                send_sem=ds.at[q], recv_sem=dr.at[q], device_id=(xor(i, order[q]), t),
                device_id_type=MESH,
            )
        )
    shared = Gather(place, norm_ref, lambda k: sseg.at[k], (sys_, syr, sps, spr), 0)
    for q in range(1, n_ep):
        sends[q].start()
    shared.start()
    stay = pltpu.make_async_copy(out_ref.at[0], seg.at[own, :, pl.ds(0, cap), :], lsem.at[0])
    stay_shared = pltpu.make_async_copy(norm_ref, sseg.at[own], lsem.at[1])
    stay.start()
    stay_shared.start()
    stay.wait()

    per_chunk = n_ep // CHUNKS
    chunk_rows = per_chunk * cap
    rows = n_ep * cap // GROUPS
    chunks = []
    for k in range(CHUNKS):
        at = functools.partial(
            lambda k, j: seg.at[j, :, pl.ds(k * chunk_rows, chunk_rows), :], k
        )
        chunks.append(Gather(place, at(own), at, (fys, fyr, fps, fpr), k))
    acts = []
    for g in range(GROUPS):
        at = functools.partial(lambda g, j: hid.at[j, :, pl.ds(g * rows, rows), :], g)
        acts.append(Gather(place, at(own), at, (hys, hyr, hps, hpr), g))
    shared_act = Gather(place, shid.at[own], lambda k: shid.at[k], (sys_, syr, sps, spr), 1)

    span = CHUNKS // GROUPS

    def begin(k):
        for q in range(k * per_chunk, (k + 1) * per_chunk):
            if q:
                sends[q].wait_recv()
        chunks[k].start()

    def gate_up(g):
        for k in range(g * CHUNKS // GROUPS, (g + 1) * CHUNKS // GROUPS):
            chunks[k].finish()
        part = pl.ds(g * rows, rows)

        @pl.loop(0, exp_dev)
        def _(e):
            gate = up = None
            for k in range(n_tp):
                x = seg[k, e, part, :]
                a = dot_t(x, gw[e, :, k * feat:(k + 1) * feat])
                b = dot_t(x, uw[e, :, k * feat:(k + 1) * feat])
                gate = a if gate is None else gate + a
                up = b if up is None else up + b
            hid[own, e, part, :] = act(gate, up)

        acts[g].start()

    per_group = n_ep // GROUPS
    returns = []

    def down(g):
        acts[g].relay()
        acts[g].finish()
        part = pl.ds(g * rows, rows)

        @pl.loop(0, exp_dev)
        def _(e):
            total = None
            for k in range(n_tp):
                a = dot(hid[k, e, part, :], dw[e, k * hidden:(k + 1) * hidden, :])
                total = a if total is None else total + a
            oexp[e, part, :] = total.astype(jnp.bfloat16)

        for q in range(g * per_group, (g + 1) * per_group):
            src = oexp.at[:, pl.ds(q * cap, cap), :]
            if q == 0:
                copy = pltpu.make_async_copy(src, ret.at[0], lsem.at[0])
            else:
                copy = pltpu.make_async_remote_copy(
                    src_ref=src, dst_ref=ret.at[q], send_sem=rs.at[q], recv_sem=rr.at[q],
                    device_id=(xor(i, order[q]), t), device_id_type=MESH,
                )
            copy.start()
            returns.append(copy)

    for k in range(span):
        begin(k)
    shared.relay()
    chunks[0].relay()
    stay_shared.wait()
    shared.finish()
    loads[0].wait()
    loads[1].wait()
    gate = up = None
    for k in range(n_tp):
        x = sseg[k]
        a = dot_t(x, sgw[:, k * feat:(k + 1) * feat])
        b = dot_t(x, suw[:, k * feat:(k + 1) * feat])
        gate = a if gate is None else gate + a
        up = b if up is None else up + b
    shid[own] = act(gate, up)
    shared_act.start()
    loads[2].wait()
    loads[3].wait()
    for k in range(1, span):
        chunks[k].relay()
    gate_up(0)
    loads[4].wait()
    loads[5].wait()
    for k in range(span, 2 * span):
        begin(k)
        chunks[k - 1].relay() if k > span else None
    down(0)
    shared_act.relay()
    for g in range(1, GROUPS):
        last = (g + 1) * span - 1
        chunks[last].relay()
        gate_up(g)
        ahead = list(range(last + 1, min(last + 1 + span, CHUNKS)))
        for k in ahead[:1] if g == 1 else ahead:
            begin(k)
        down(g)
        for k in ahead[1:] if g == 1 else ():
            begin(k)
        for k in ahead[:-1]:
            chunks[k].relay()
    shared_act.finish()
    total = None
    for k in range(n_tp):
        a = dot(shid[k], sdw[k * s_hidden:(k + 1) * s_hidden, :])
        total = a if total is None else total + a
    res_ref[...] = total
    width = per_group * exp_dev * cap
    for g in range(GROUPS):
        for q in range(g * per_group, (g + 1) * per_group):
            if q:
                returns[q].wait_recv()
            else:
                returns[q].wait()
        piece = ret[g * per_group:(g + 1) * per_group].reshape(width, feat)
        cols = pl.ds(g * width, width)
        res_ref[...] += dot(whi_ref[:, cols], piece) + dot(wlo_ref[:, cols], piece)
    for q in range(1, n_ep):
        sends[q].wait_send()
        returns[q].wait_send()
    for gather in chunks + acts + [shared, shared_act]:
        gather.drain()


def exchange(n_ep, n_tp, outgoing, normed, whi, wlo, gate, up, down, s_gate, s_up, s_down):
    exp_dev, hidden, width = gate.shape
    _, _, cap, feat = outgoing.shape
    tok = normed.shape[0]
    s_hidden = s_gate.shape[0]
    n_y = n_tp // 2
    bf = jnp.bfloat16
    dma = pltpu.SemaphoreType.DMA
    far, near = n_y - 1, n_y
    vmem, hbm = pl.BlockSpec(memory_space=pltpu.VMEM), pl.BlockSpec(memory_space=pl.ANY)
    return pl.pallas_call(
        functools.partial(kernel, n_ep, n_tp),
        out_shape=jax.ShapeDtypeStruct((tok, feat), jnp.float32),
        in_specs=[vmem] * 4 + [hbm] * 6,
        out_specs=vmem,
        scratch_shapes=[
            pltpu.VMEM((n_tp, exp_dev, n_ep * cap, feat), bf),
            pltpu.VMEM((n_tp, tok, feat), bf),
            pltpu.VMEM((n_tp, exp_dev, n_ep * cap, hidden), bf),
            pltpu.VMEM((n_tp, tok, s_hidden), bf),
            pltpu.VMEM((exp_dev, n_ep * cap, feat), bf),
            pltpu.VMEM((n_ep, exp_dev, cap, feat), bf),
            pltpu.VMEM(gate.shape, bf),
            pltpu.VMEM(up.shape, bf),
            pltpu.VMEM(down.shape, bf),
            pltpu.VMEM(s_gate.shape, bf),
            pltpu.VMEM(s_up.shape, bf),
            pltpu.VMEM(s_down.shape, bf),
            dma((6,)), dma((2,)),
            dma((n_ep,)), dma((n_ep,)), dma((n_ep,)), dma((n_ep,)),
            dma((CHUNKS * far,)), dma((CHUNKS * far,)), dma((CHUNKS * near,)), dma((CHUNKS * near,)),
            dma((GROUPS * far,)), dma((GROUPS * far,)), dma((GROUPS * near,)), dma((GROUPS * near,)),
            dma((2 * far,)), dma((2 * far,)), dma((2 * near,)), dma((2 * near,)),
        ],
        compiler_params=pltpu.CompilerParams(
            collective_id=0, has_side_effects=True, vmem_limit_bytes=56 * 1024 * 1024
        ),
    )(outgoing, normed, whi, wlo, gate, up, down, s_gate, s_up, s_down)


def total_over_tp(values):
    return jnp.sum(lax.all_gather(values, "tp"), axis=0)


def on_device(
    n_ep, n_tp, tokens, pre_gain, expert_ids, route_weight, expert_gate, expert_up, expert_down,
    shared_gate, shared_up, shared_down, out_gain,
):
    tok_count, top_count = expert_ids.shape
    exp_dev = expert_gate.shape[0]
    width = expert_gate.shape[2]
    experts = exp_dev * n_ep
    capacity = 4 * tok_count * top_count // (3 * experts)
    feat = tokens.shape[1]
    tok_float = tokens.astype(jnp.float32)
    square_sum = total_over_tp(jnp.sum(tok_float * tok_float, axis=1))
    normed = (tok_float * lax.rsqrt(square_sum[:, None] / width + EPSILON) * pre_gain).astype(
        jnp.bfloat16
    )
    i = lax.axis_index("ep")
    steps = jnp.array(step_order(n_ep), jnp.int32)
    names = ((i ^ steps)[:, None] * exp_dev + jnp.arange(exp_dev, dtype=jnp.int32)).reshape(experts)
    same = expert_ids[:, :, None] == names[None, None, :]
    member = jnp.any(same, axis=1)
    weight = jnp.sum(jnp.where(same, route_weight[:, :, None], 0.0), axis=1)
    row = jnp.arange(tok_count, dtype=jnp.int32)
    earlier = (row[None, :] < row[:, None]).astype(jnp.bfloat16)
    before = jnp.dot(earlier, member.astype(jnp.bfloat16), preferred_element_type=jnp.float32)
    slot = jnp.where(member, before.astype(jnp.int32), -1)
    places = jnp.arange(capacity, dtype=jnp.int32)
    pick = (slot.T[:, None, :] == places[None, :, None]).astype(jnp.bfloat16)
    outgoing = jnp.dot(
        pick.reshape(experts * capacity, tok_count), normed, preferred_element_type=jnp.float32
    ).astype(jnp.bfloat16)
    outgoing = outgoing.reshape(n_ep, exp_dev, capacity, feat)
    high = lax.reduce_precision(weight, 8, 7)
    low = weight - high
    here = slot[:, :, None] == places[None, None, :]

    def spread(values):
        return jnp.where(here, values[:, :, None], 0.0).astype(jnp.bfloat16).reshape(
            tok_count, experts * capacity
        )

    summed = exchange(
        n_ep, n_tp, outgoing, normed, spread(high), spread(low), expert_gate, expert_up,
        expert_down, shared_gate, shared_up, shared_down,
    )
    out_square = total_over_tp(jnp.sum(summed * summed, axis=1))
    return (summed * lax.rsqrt(out_square[:, None] / width + EPSILON) * out_gain).astype(
        jnp.bfloat16
    )


def solution(mesh):
    return jax.shard_map(
        functools.partial(on_device, mesh.shape["ep"], mesh.shape["tp"]),
        mesh=mesh,
        in_specs=(
            P("ep", "tp"),
            P("tp"),
            P("ep", None),
            P("ep", None),
            P("ep", "tp", None),
            P("ep", "tp", None),
            P("ep", None, "tp"),
            P("tp", None),
            P("tp", None),
            P(None, "tp"),
            P("tp"),
        ),
        out_specs=P("ep", "tp"),
        check_vma=False,
    )
```
